32 devices in a mesh: sp: 8 (over z, y), tp: 4 (over x, core).
Axes of the slice: x: 2, y: 2, z: 4, core: 2. Of those that a mesh axis runs over, the one named last changes fastest.
Arguments:
- queries: bfloat16 [4096, 2048], P('sp', 'tp'), may hold values from -8 to 8
- keys: bfloat16 [4096, 512], P('sp', 'tp'), may hold values from -8 to 8
- values: bfloat16 [4096, 512], P('sp', 'tp'), may hold values from -6 to 6
- q_gain: float32 [128], replicated, may hold values from 0.1 to 5.8
- k_gain: float32 [128], replicated, may hold values from 0.1 to 5.8
- out_weight: bfloat16 [2048, 2048], replicated, may hold values from -0.125 to 0.125
- out_gain: float32 [2048], replicated, may hold values from 0.1 to 1.9
- residual_in: bfloat16 [4096, 2048], P(('sp', 'tp')), may hold values from -6 to 6
- mlp_gain: float32 [2048], replicated, may hold values from 0.1 to 1.9
- gate_weight: bfloat16 [2048, 5632], P('sp', 'tp'), may hold values from -0.125 to 0.125
- up_weight: bfloat16 [2048, 5632], P('sp', 'tp'), may hold values from -0.125 to 0.125
- down_weight: bfloat16 [5632, 2048], P('tp', 'sp'), may hold values from -0.078125 to 0.078125
- final_gain: float32 [2048], replicated, may hold values from 0.1 to 1.9
Outputs:
- layer_out: bfloat16 [4096, 2048], P(('sp', 'tp'))
The draws below stay inside these ranges and needn't reach their ends.
All inputs are finite; a program needn't handle non-finite values.
Results may differ from the reference program's by a relative error of at most 0.015.
The reference program's roundings to bfloat16 on the way count: a program that leaves them out, or rounds other values in their place, can miss the bound.
Values may be sent and summed in bfloat16 or wider, within the bound.
No kernel may reach another device: no remote copies, remote signals or barrier semaphores. Data moves between devices by JAX's collectives and lax.ppermute only.
A program may use at most 128 MiB of HBM per device.

```python
import jax
import jax.numpy as jnp
from jax import lax

D = 2048
HQ = 16
KV = 4
HD = 128
FF = 5632
GRID_W = 64
TOK_DEV = 512
TOKENS = 4096


def drawn(base_key):
    query_base = jnp.clip(jax.random.normal(jax.random.fold_in(base_key, 101), (TOKENS, HQ, HD), jnp.float32), -6.0, 6.0)
    key_base = jnp.clip(jax.random.normal(jax.random.fold_in(base_key, 102), (TOKENS, KV, HD), jnp.float32), -6.0, 6.0)
    return (query_base.reshape(TOKENS, HQ * HD), key_base.reshape(TOKENS, KV * HD))


def gain_values(base_key):
    return 1.0 + 0.18 * jnp.clip(jax.random.normal(base_key, (HD,), jnp.float32), -5.0, 5.0)


def draw_queries(key, part):
    return drawn(key)[0].astype(jnp.bfloat16)


def draw_keys(key, part):
    return drawn(key)[1].astype(jnp.bfloat16)


def draw_q_gain(key, part):
    return gain_values(jax.random.fold_in(key, 201))


def draw_k_gain(key, part):
    return gain_values(jax.random.fold_in(key, 202))


def level_of(own_key, shape, shards, smallest, largest):
    gain, own = 1.0, jax.random.fold_in(own_key, 6)
    for position, shards_of in shards:
        draws = jnp.exp(jax.random.uniform(jax.random.fold_in(own, position), (shards_of,), jnp.float32, smallest / len(shards), largest / len(shards)))
        gain = gain * jnp.repeat(draws, shape[position] // shards_of).reshape([-1 if axis == position else 1 for axis in range(len(shape))])
    return gain


def scatter_about(key, extent, spread, bound, shards=(), kind=jnp.bfloat16):
    loudness = level_of(key, extent, shards, -0.22, 0.18) if shards else 1.0
    entries = jax.random.normal(key, extent, jnp.float32) * spread * loudness
    return jnp.minimum(jnp.maximum(entries, -bound), bound).astype(kind)


def setup_inputs(seed: int = 0) -> dict:
    splits = jax.random.split(jax.random.key(seed), 14)
    queries = draw_queries(jax.random.fold_in(splits[13], 71), 0)
    keys = draw_keys(jax.random.fold_in(splits[13], 71), 0)
    values = scatter_about(splits[2], (TOKENS, KV * HD), 1.0, 6.0, ((0, 8), (1, 4)))
    q_gain = draw_q_gain(jax.random.fold_in(splits[13], 71), 0)
    k_gain = draw_k_gain(jax.random.fold_in(splits[13], 71), 0)
    out_weight = scatter_about(splits[5], (HQ * HD, D), (HQ * HD) ** -0.5, 0.125)
    out_gain = jnp.clip(1.0 + 0.18 * jax.random.normal(splits[6], (D,), jnp.float32), 0.1, 1.9)
    residual_in = scatter_about(splits[7], (TOKENS, D), 1.0, 6.0, ((0, 32),))
    mlp_gain = jnp.clip(1.0 + 0.18 * jax.random.normal(splits[8], (D,), jnp.float32), 0.1, 1.9)
    gate_weight = scatter_about(splits[9], (D, FF), D ** -0.5, 0.125, ((0, 8), (1, 4)))
    up_weight = scatter_about(splits[10], (D, FF), D ** -0.5, 0.125, ((0, 8), (1, 4)))
    down_weight = scatter_about(splits[11], (FF, D), FF ** -0.5, 0.078125, ((0, 4), (1, 8)))
    final_gain = jnp.clip(1.0 + 0.18 * jax.random.normal(splits[12], (D,), jnp.float32), 0.1, 1.9)
    return dict(queries=queries, keys=keys, values=values, q_gain=q_gain, k_gain=k_gain, out_weight=out_weight, out_gain=out_gain, residual_in=residual_in, mlp_gain=mlp_gain, gate_weight=gate_weight, up_weight=up_weight, down_weight=down_weight, final_gain=final_gain)


def rms_scale(matrix):
    return matrix * lax.rsqrt(lax.optimization_barrier(jnp.mean(matrix * matrix, axis=-1, keepdims=True)) + 1e-06)

def rotary(matrix, positions):
    quarter = matrix.shape[-1] // 4
    freqs = 10000.0 ** (-jnp.arange(quarter, dtype=jnp.float32) / quarter)
    grid = jnp.stack([positions // GRID_W, positions % GRID_W], axis=-1).astype(jnp.float32)
    angle = grid[:, :, None] * freqs
    cosine = jnp.cos(angle)[:, None]
    sine = jnp.sin(angle)[:, None]
    parts = matrix.reshape(matrix.shape[:-1] + (2, 2, quarter))
    first = parts[..., 0, :]
    second = parts[..., 1, :]
    turned = jnp.stack([first * cosine - second * sine, second * cosine + first * sine], axis=-2)
    return turned.reshape(matrix.shape)

def reference(queries, keys, values, q_gain, k_gain, out_weight, out_gain, residual_in, mlp_gain, gate_weight, up_weight, down_weight, final_gain):
    tok_total = queries.shape[0]
    positions = jnp.arange(tok_total, dtype=jnp.int32)
    query_rot = rotary(rms_scale(queries.reshape(tok_total, HQ, HD).astype(jnp.float32)) * q_gain, positions).astype(jnp.bfloat16)
    key_rot = rotary(rms_scale(keys.reshape(tok_total, KV, HD).astype(jnp.float32)) * k_gain, positions).astype(jnp.bfloat16)
    value_heads = values.reshape(tok_total, KV, HD)
    group_size = HQ // KV
    score_scale = HD ** (-0.5)

    def one_head(head_index):
        query_head = lax.dynamic_index_in_dim(query_rot, head_index, 1, keepdims=False)
        key_head = lax.dynamic_index_in_dim(key_rot, head_index // group_size, 1, keepdims=False)
        value_head = lax.dynamic_index_in_dim(value_heads, head_index // group_size, 1, keepdims=False)

        def one_block(query_block):
            scores = jnp.dot(query_block, key_head.T, preferred_element_type=jnp.float32) * score_scale
            highest = lax.optimization_barrier(jnp.max(scores, axis=-1, keepdims=True))
            exp_scores = jnp.exp(scores - highest)
            weight_sum = lax.optimization_barrier(jnp.sum(exp_scores, axis=-1, keepdims=True))
            mixed = jnp.dot(exp_scores.astype(jnp.bfloat16), value_head, preferred_element_type=jnp.float32) / weight_sum
            return mixed.astype(jnp.bfloat16)
        blocks = query_head.reshape(tok_total // TOK_DEV, TOK_DEV, HD)
        return lax.map(one_block, blocks).reshape(tok_total, HD)
    per_head = lax.map(one_head, jnp.arange(HQ, dtype=jnp.int32))
    attended = jnp.transpose(per_head, (1, 0, 2)).reshape(tok_total, HQ * HD)
    projected = jnp.dot(attended, out_weight, preferred_element_type=jnp.float32)
    mid_stream = (residual_in.astype(jnp.float32) + out_gain * rms_scale(projected)).astype(jnp.bfloat16)
    normed = (mlp_gain * rms_scale(mid_stream.astype(jnp.float32))).astype(jnp.bfloat16)
    gate_proj = jnp.dot(normed, gate_weight, preferred_element_type=jnp.float32)
    up_proj = jnp.dot(normed, up_weight, preferred_element_type=jnp.float32)
    hidden = (jax.nn.silu(gate_proj) * up_proj).astype(jnp.bfloat16)
    mlp_branch = jnp.dot(hidden, down_weight, preferred_element_type=jnp.float32)
    return (mid_stream.astype(jnp.float32) + final_gain * rms_scale(mlp_branch)).astype(jnp.bfloat16)
```

```python
import functools
import math

import jax
import jax.numpy as jnp
from jax import lax
from jax.experimental import pallas as pl
from jax.experimental.pallas import tpu as pltpu
from jax.sharding import PartitionSpec as P

GRID_W = 64
LANES = 128


def rms_scale(matrix):
    return matrix * lax.rsqrt(jnp.mean(matrix * matrix, axis=-1, keepdims=True) + 1e-06)


def rotary(matrix, positions):
    quarter = matrix.shape[-1] // 4
    freqs = 10000.0 ** (-jnp.arange(quarter, dtype=jnp.float32) / quarter)
    grid = jnp.stack([positions // GRID_W, positions % GRID_W], axis=-1).astype(jnp.float32)
    angle = grid[:, :, None] * freqs
    cosine = jnp.cos(angle)[:, None]
    sine = jnp.sin(angle)[:, None]
    parts = matrix.reshape(matrix.shape[:-1] + (2, 2, quarter))
    first = parts[..., 0, :]
    second = parts[..., 1, :]
    turned = jnp.stack([first * cosine - second * sine, second * cosine + first * sine], axis=-2)
    return turned.reshape(matrix.shape)


def attention_block(scale, q_ref, k_ref, v_ref, o_ref):
    scores = lax.dot_general(
        q_ref[...], k_ref[...], (((1,), (1,)), ((), ())), preferred_element_type=jnp.float32
    )
    highest = jnp.max(scores, axis=-1, keepdims=True)
    weights = jnp.exp2((scores - highest) * scale)
    total = jnp.sum(weights, axis=-1, keepdims=True)
    mixed = jnp.dot(weights.astype(jnp.bfloat16), v_ref[...], preferred_element_type=jnp.float32)
    o_ref[...] = (mixed / total).astype(o_ref.dtype)


def attention(query, key_value, head_size):
    rows, width = query.shape
    total = key_value.shape[0]
    q_heads = width // head_size
    kv_heads = key_value.shape[1] // (2 * head_size)
    group = q_heads // kv_heads
    block = math.gcd(rows, 256)
    scale = head_size ** (-0.5) * math.log2(math.e)
    return pl.pallas_call(
        functools.partial(attention_block, scale),
        grid=(q_heads, rows // block),
        in_specs=[
            pl.BlockSpec((block, head_size), lambda h, i: (i, h)),
            pl.BlockSpec((total, head_size), lambda h, i: (0, h // group)),
            pl.BlockSpec((total, head_size), lambda h, i: (0, kv_heads + h // group)),
        ],
        out_specs=pl.BlockSpec((block, head_size), lambda h, i: (i, h)),
        out_shape=jax.ShapeDtypeStruct((rows, width), jnp.bfloat16),
        cost_estimate=pl.CostEstimate(
            flops=4 * rows * width * total,
            transcendentals=rows * q_heads * total,
            bytes_accessed=4 * rows * width + 4 * total * head_size,
        ),
        name="attention",
    )(query, key_value, key_value)


def swap(array, axis, size, bit):
    return lax.ppermute(array, axis, [(i, i ^ bit) for i in range(size)])


def ring_pieces(own, size, split_axes):
    ring = size // 2
    up = [(i, (i + 2) % size) for i in range(size)]
    down = [(i, (i - 2) % size) for i in range(size)]
    pieces = {0: own}
    from_low, from_high = own, own
    for hop in range(1, (ring - 1) // 2 + 1):
        from_low = [lax.ppermute(a, "sp", up) for a in from_low]
        from_high = [lax.ppermute(a, "sp", down) for a in from_high]
        pieces[ring - hop] = from_low
        pieces[hop] = from_high
    if ring % 2 == 0:
        far = []
        for low, high, axis in zip(from_low, from_high, split_axes):
            half = low.shape[axis] // 2
            head = lax.ppermute(lax.slice_in_dim(low, 0, half, axis=axis), "sp", up)
            tail = lax.ppermute(
                lax.slice_in_dim(high, half, high.shape[axis], axis=axis), "sp", down
            )
            far.append((head, tail))
        pieces[ring // 2] = far
    out = []
    for position, axis in enumerate(split_axes):
        parts = []
        for k in range(ring):
            piece = pieces[k][position]
            parts.extend(piece if isinstance(piece, tuple) else (piece,))
        out.append(jnp.concatenate(parts, axis=axis))
    return out


def roll_columns(matrix, shift):
    width = matrix.shape[-1]
    return lax.dynamic_slice_in_dim(
        jnp.concatenate([matrix, matrix], axis=-1), shift, width, axis=matrix.ndim - 1
    )


def make_body(sp, tp):
    def on_device(
        queries,
        keys,
        values,
        q_gain,
        k_gain,
        out_weight,
        out_gain,
        residual_in,
        mlp_gain,
        gate_weight,
        up_weight,
        down_weight,
        final_gain,
    ):
        tok_rows = queries.shape[0]
        head_size = q_gain.shape[0]
        q_heads = queries.shape[1] // head_size
        kv_heads = keys.shape[1] // head_size
        index = lax.axis_index("sp")
        side = index % 2
        outer = index // 2
        first_side = side == 0
        positions = index * tok_rows + jnp.arange(tok_rows, dtype=jnp.int32)

        key_rot = rotary(
            rms_scale(keys.reshape(tok_rows, kv_heads, head_size).astype(jnp.float32)) * k_gain,
            positions,
        ).astype(jnp.bfloat16)
        key_value = jnp.concatenate(
            [key_rot.reshape(tok_rows, kv_heads * head_size), values], axis=1
        )
        key_value_pair = jnp.concatenate([key_value, swap(key_value, "sp", sp, 1)], axis=0)

        half = gate_weight.shape[1] // 2
        main = half // LANES * LANES
        rest = half - main

        def half_of(which):
            def cut(matrix, k):
                a = lax.slice_in_dim(matrix, k * main, (k + 1) * main, axis=1)
                b = lax.slice_in_dim(
                    matrix, 2 * main + k * rest, 2 * main + (k + 1) * rest, axis=1
                )
                return a, b

            def both(k):
                ga, gb = cut(gate_weight, k)
                ua, ub = cut(up_weight, k)
                return jnp.concatenate([ga, ua, gb, ub], axis=1)

            def rows(k):
                return jnp.concatenate(
                    [
                        lax.slice_in_dim(down_weight, k * main, (k + 1) * main, axis=0),
                        lax.slice_in_dim(
                            down_weight, 2 * main + k * rest, 2 * main + (k + 1) * rest, axis=0
                        ),
                    ],
                    axis=0,
                )

            return jnp.where(which, both(0), both(1)), jnp.where(which, rows(0), rows(1))

        kept = half_of(first_side)
        sent = half_of(jnp.logical_not(first_side))
        key_value_pair, sent = lax.optimization_barrier((key_value_pair, sent))
        got = [swap(a, "sp", sp, 1) for a in sent]
        own_pair = [
            jnp.where(
                first_side,
                jnp.concatenate([k, g], axis=axis),
                jnp.concatenate([g, k], axis=axis),
            )
            for k, g, axis in zip(kept, got, (0, 1))
        ]
        (key_value_all,) = ring_pieces([key_value_pair], sp, (0,))

        query_rot = (
            rotary(
                rms_scale(queries.reshape(tok_rows, q_heads, head_size).astype(jnp.float32))
                * q_gain,
                positions,
            )
            .astype(jnp.bfloat16)
            .reshape(tok_rows, q_heads * head_size)
        )
        key_value_all, own_pair = lax.optimization_barrier((key_value_all, own_pair))
        gate_up, down_full = ring_pieces(own_pair, sp, (0, 1))

        attended = attention(query_rot, key_value_all, head_size)
        head_rows = lax.all_to_all(attended, "tp", split_axis=0, concat_axis=1, tiled=True)
        projected = jnp.dot(head_rows, out_weight, preferred_element_type=jnp.float32)
        mid_stream = (residual_in.astype(jnp.float32) + out_gain * rms_scale(projected)).astype(
            jnp.bfloat16
        )
        normed = (mlp_gain * rms_scale(mid_stream.astype(jnp.float32))).astype(jnp.bfloat16)

        width = normed.shape[1]
        shift = outer * (width // (sp // 2))
        normed = roll_columns(normed, shift)

        rows = normed.shape[0]
        part = rows // 2
        by_x = lambda a: swap(a, "tp", tp, tp // 2)
        by_y = lambda a: swap(a, "sp", sp, 1)
        by_core = lambda a: swap(a, "tp", tp, 1)
        first, second = normed[:part], normed[part:]
        first = jnp.concatenate([first, by_x(first)], axis=0)
        second = jnp.concatenate([second, by_y(second)], axis=0)
        first = jnp.concatenate([first, by_y(first)], axis=0)
        second = jnp.concatenate([second, by_x(second)], axis=0)
        near = jnp.concatenate([first, second], axis=0)
        mixer_in = jnp.concatenate([near, by_core(near)], axis=0)

        both = jnp.dot(mixer_in, gate_up, preferred_element_type=jnp.float32)
        hidden = jnp.concatenate(
            [
                (jax.nn.silu(both[:, :main]) * both[:, main : 2 * main]).astype(jnp.bfloat16),
                (
                    jax.nn.silu(both[:, 2 * main : 2 * main + rest])
                    * both[:, 2 * main + rest :]
                ).astype(jnp.bfloat16),
            ],
            axis=1,
        )
        partial = jnp.dot(hidden, down_full, preferred_element_type=jnp.float32).astype(
            jnp.bfloat16
        )

        def add(a, b):
            return (a.astype(jnp.float32) + b.astype(jnp.float32)).astype(jnp.bfloat16)

        group = near.shape[0]
        near_sum = add(partial[:group], by_core(partial[group:]))
        quarter = group // 4
        first, second = near_sum[: 2 * quarter], near_sum[2 * quarter :]
        first = add(first[:quarter], by_y(first[quarter:]))
        second = add(second[:quarter], by_x(second[quarter:]))
        first = add(first[:part], by_x(first[part:]))
        second = add(second[:part], by_y(second[part:]))
        mlp_branch = jnp.concatenate([first, second], axis=0)
        mlp_branch = roll_columns(mlp_branch, width - shift).astype(jnp.float32)
        return (mid_stream.astype(jnp.float32) + final_gain * rms_scale(mlp_branch)).astype(
            jnp.bfloat16
        )

    return on_device


def solution(mesh):
    return jax.shard_map(
        make_body(mesh.shape["sp"], mesh.shape["tp"]),
        mesh=mesh,
        in_specs=(
            P("sp", "tp"),
            P("sp", "tp"),
            P("sp", "tp"),
            P(),
            P(),
            P(),
            P(),
            P(("sp", "tp"), None),
            P(),
            P("sp", "tp"),
            P("sp", "tp"),
            P("tp", "sp"),
            P(),
        ),
        out_specs=P(("sp", "tp"), None),
        check_vma=False,
    )
```
